32 devices in a mesh: rep: 4 (over z), fs: 2 (over y), tp: 4 (over x, core).
Axes of the slice: x: 2, y: 2, z: 4, core: 2. Of those that a mesh axis runs over, the one named last changes fastest.
Arguments:
- tokens: bfloat16 [3072, 2048], P('rep', 'fs'), may hold values from -6 to 6
- gate_pre: bfloat16 [3072, 6144], P('rep', 'tp'), may hold values from -6 to 6
- up_pre: bfloat16 [3072, 6144], P('rep', 'tp'), may hold values from -6 to 6
- hidden_grad: bfloat16 [3072, 6144], P('rep', 'tp'), may hold values from -0.75 to 0.75
- gate_weight: bfloat16 [2048, 6144], P('fs', 'tp'), may hold values from -0.125 to 0.125
- up_weight: bfloat16 [2048, 6144], P('fs', 'tp'), may hold values from -0.125 to 0.125
- gate_taps: float32 [3, 6144], P(None, 'tp'), may hold values from -3.5 to 3.5
- up_taps: float32 [3, 6144], P(None, 'tp'), may hold values from -3.5 to 3.5
- gate_bias: float32 [6144], P('tp'), may hold values from -4 to 4
- up_bias: float32 [6144], P('tp'), may hold values from -4 to 4
Outputs:
- input_grad: bfloat16 [3072, 2048], P('rep', 'fs')
- gate_weight_grad: float32 [2048, 6144], P('fs', 'tp')
- up_weight_grad: float32 [2048, 6144], P('fs', 'tp')
- gate_taps_grad: float32 [3, 6144], P(None, 'tp')
- up_taps_grad: float32 [3, 6144], P(None, 'tp')
- gate_bias_grad: float32 [6144], P('tp')
- up_bias_grad: float32 [6144], P('tp')
The draws below stay inside these ranges and needn't reach their ends.
All inputs are finite; a program needn't handle non-finite values.
Results may differ from the reference program's by a relative error of at most 0.017.
Values may be sent and summed in bfloat16 or wider, within the bound.
A program may use at most 64 MiB of HBM per device.

```python
import jax
import jax.numpy as jnp
from jax import lax

D = 2048
FF = 6144
TAPS = 3
SEQ_LEN = 768
TOKENS = 3072
N_REP = 4
N_TP = 4


def strengthened(entries, stream_key, source, target, blocks, factor):
    def block_of(dim):
        return (jnp.arange(entries.shape[dim]) // (entries.shape[dim] // blocks)).reshape((-1,) + (1,) * (entries.ndim - 1 - dim))

    near = jax.random.permutation(stream_key, blocks)[block_of(target)]
    second = (block_of(target) + blocks // 2) % blocks
    return jnp.where((block_of(source) == near) | (block_of(source) == second), factor * entries, entries)


def level_of(own_key, shape, split, low, high):
    gain = 1.0
    for position, blocks in split:
        draws = jax.random.uniform(jax.random.fold_in(jax.random.fold_in(own_key, 6), position), (blocks,), jnp.float32, low / len(split), high / len(split))
        gain = gain * jnp.repeat(jnp.exp(draws), shape[position] // blocks).reshape((-1,) + (1,) * (len(shape) - 1 - position))
    return gain


def noise(own_key, dims, width, most, split=(), kind=jnp.bfloat16):
    gain = level_of(own_key, dims, split, -0.22, 0.18) if split else 1.0
    values = jax.random.normal(own_key, dims, jnp.float32) * width * gain
    return jnp.minimum(jnp.maximum(values, -most), most).astype(kind)


def bell_draw_with(stream_key, dims, spread, bound, split, heavy, held_as=jnp.bfloat16):
    array = spread * jax.random.normal(stream_key, dims, jnp.float32)
    if split:
        array = array * level_of(stream_key, dims, split, -0.22, 0.18)
    return jnp.clip(strengthened(array, jax.random.fold_in(stream_key, 3), *heavy), -bound, bound).astype(held_as)


def setup_inputs(seed: int = 0) -> dict:
    key_list = jax.random.split(jax.random.key(seed), 11)
    tokens = noise(key_list[0], (TOKENS, D), 1.0, 6.0, ((0, 4), (1, 2)))
    gate_pre = noise(key_list[1], (TOKENS, FF), 1.0, 6.0, ((0, 4), (1, 4)))
    up_pre = noise(key_list[2], (TOKENS, FF), 1.0, 6.0, ((0, 4), (1, 4)))
    hidden_grad = bell_draw_with(key_list[3], (TOKENS, FF), 0.125, 0.75, ((0, 4), (1, 4)), (1, 0, 4, 2.0))
    gate_weight = noise(key_list[4], (D, FF), D ** -0.5, 0.125, ((0, 2), (1, 4)))
    up_weight = noise(key_list[5], (D, FF), D ** -0.5, 0.125, ((0, 2), (1, 4)))
    gate_taps = noise(key_list[6], (TAPS, FF), TAPS ** -0.5, 3.5, ((1, 4),), jnp.float32)
    up_taps = noise(key_list[7], (TAPS, FF), TAPS ** -0.5, 3.5, ((1, 4),), jnp.float32)
    gate_bias = noise(key_list[8], (FF,), 1.0, 4.0, ((0, 4),), jnp.float32)
    up_bias = noise(key_list[9], (FF,), 1.0, 4.0, ((0, 4),), jnp.float32)
    return dict(tokens=tokens, gate_pre=gate_pre, up_pre=up_pre, hidden_grad=hidden_grad, gate_weight=gate_weight, up_weight=up_weight, gate_taps=gate_taps, up_taps=up_taps, gate_bias=gate_bias, up_bias=up_bias)


def causal_mix(signal, tap_weights):
    tap_count = tap_weights.shape[0]
    length = signal.shape[0]
    padded = jnp.pad(signal, ((tap_count - 1, 0), (0, 0)))
    mixed = padded[0:length] * tap_weights[0]
    for offset in range(1, tap_count):
        mixed = mixed + padded[offset:offset + length] * tap_weights[offset]
    return mixed


def mix_back(signal, tap_weights):
    tap_count = tap_weights.shape[0]
    length = signal.shape[0]
    padded = jnp.pad(signal, ((0, tap_count - 1), (0, 0)))
    begin = tap_count - 1
    mixed = padded[begin:begin + length] * tap_weights[0]
    for offset in range(1, tap_count):
        begin = tap_count - 1 - offset
        mixed = mixed + padded[begin:begin + length] * tap_weights[offset]
    return mixed


def tap_terms(grad_signal, signal, tap_count):
    length = signal.shape[0]
    padded = jnp.pad(signal, ((tap_count - 1, 0), (0, 0)))
    return jnp.stack([jnp.sum(grad_signal * padded[offset:offset + length], axis=0) for offset in range(tap_count)])


def backward_terms(gate_pre, up_pre, hidden_grad, gate_taps, up_taps, gate_bias, up_bias):
    gate_float = gate_pre.astype(jnp.float32)
    up_float = up_pre.astype(jnp.float32)
    gate_mixed = causal_mix(gate_float, gate_taps) + gate_bias
    up_mixed = causal_mix(up_float, up_taps) + up_bias
    logistic = jax.nn.sigmoid(gate_mixed)
    cotangent = hidden_grad.astype(jnp.float32)
    gate_delta = cotangent * up_mixed * logistic * (1.0 + gate_mixed * (1.0 - logistic))
    up_delta = cotangent * gate_mixed * logistic
    gate_back = mix_back(gate_delta, gate_taps).astype(jnp.bfloat16)
    up_back = mix_back(up_delta, up_taps).astype(jnp.bfloat16)
    tap_count = gate_taps.shape[0]
    return (gate_back, up_back, tap_terms(gate_delta, gate_float, tap_count),
            tap_terms(up_delta, up_float, tap_count), jnp.sum(gate_delta, axis=0), jnp.sum(up_delta, axis=0))


def reference(tokens, gate_pre, up_pre, hidden_grad, gate_weight, up_weight, gate_taps, up_taps, gate_bias, up_bias):
    seq_shape = (N_REP, SEQ_LEN, FF)

    def per_sequence(packed):
        return backward_terms(packed[0], packed[1], packed[2], gate_taps, up_taps, gate_bias, up_bias)

    seq_parts = lax.map(per_sequence, (gate_pre.reshape(seq_shape), up_pre.reshape(seq_shape), hidden_grad.reshape(seq_shape)))
    gate_back = seq_parts[0].reshape(TOKENS, FF)
    up_back = seq_parts[1].reshape(TOKENS, FF)
    block_width = FF // N_TP

    def add_block(total, block_index):
        start = (block_index * block_width).astype(jnp.int32)
        gate_cols = lax.dynamic_slice_in_dim(gate_back, start, block_width, 1)
        up_cols = lax.dynamic_slice_in_dim(up_back, start, block_width, 1)
        gate_rows = lax.dynamic_slice_in_dim(gate_weight, start, block_width, 1)
        up_rows = lax.dynamic_slice_in_dim(up_weight, start, block_width, 1)
        block_term = (jnp.dot(gate_cols, gate_rows.T, preferred_element_type=jnp.float32)
                      + jnp.dot(up_cols, up_rows.T, preferred_element_type=jnp.float32)).astype(jnp.bfloat16)
        return total + block_term.astype(jnp.float32), None

    summed, _ = lax.scan(add_block, jnp.zeros((TOKENS, D), jnp.float32), jnp.arange(N_TP, dtype=jnp.int32))
    input_grad = summed.astype(jnp.bfloat16)
    gate_weight_grad = jnp.dot(tokens.T, gate_back, preferred_element_type=jnp.float32)
    up_weight_grad = jnp.dot(tokens.T, up_back, preferred_element_type=jnp.float32)
    return (input_grad, gate_weight_grad, up_weight_grad, jnp.sum(seq_parts[2], axis=0),
            jnp.sum(seq_parts[3], axis=0), jnp.sum(seq_parts[4], axis=0), jnp.sum(seq_parts[5], axis=0))
```

```python
import functools

import jax
import jax.numpy as jnp
from jax import lax
from jax.experimental import pallas as pl
from jax.experimental.pallas import tpu as pltpu
from jax.sharding import PartitionSpec as P

MESH = pl.DeviceIdType.MESH
CW = 128
NQ = 8
PAD = 8
TICKS = 4
LAG = 4
TILE = 32
F32 = jnp.float32
BF16 = jnp.bfloat16


def schedule(blocks, rep_count):
    done = max(blocks - 1, 0)
    last_tick = blocks * NQ + LAG * (rep_count - 1)
    steps = max(-(-last_tick // TICKS), done + rep_count, done + 5)
    return done, steps


def fused(
    rep_count,
    tp_count,
    tokens,
    gate_pre,
    up_pre,
    hidden,
    gate_weight,
    up_weight,
    gate_taps,
    up_taps,
    gate_bias,
    up_bias,
    own,
    final,
    small_out,
    tok,
    tok_t,
    gpre,
    upre,
    hid,
    gw,
    uw,
    gpad,
    upad,
    gdel,
    udel,
    gback,
    uback,
    parts_ref,
    acc,
    from_left,
    from_right,
    to_left,
    term,
    term_in,
    small,
    small_from_left,
    small_from_right,
    small_to_right,
    small_to_left,
    load_sem,
    weight_sem,
    send_r,
    recv_r,
    send_l,
    recv_l,
    scatter_send,
    scatter_recv,
    gather_send,
    gather_recv,
    small_sem,
):
    z = lax.axis_index("rep")
    me = lax.axis_index("tp")
    length, hidden_cols = gate_pre.shape
    width = tokens.shape[1]
    blocks = hidden_cols // CW
    chunks = blocks * NQ
    rows_q = width // NQ
    taps = gate_taps.shape[0]
    done, steps = schedule(blocks, rep_count)
    has_left = z > 0
    has_right = z < rep_count - 1
    both = has_left & has_right

    def columns(b):
        return pl.ds(pl.multiple_of(b * CW, CW), CW)

    def load(which, b):
        src = (gate_pre, up_pre, hidden)[which]
        dst = (gpre, upre, hid)[which]
        return pltpu.make_async_copy(
            src.at[:, columns(b)], dst.at[b], load_sem.at[which, b]
        )

    token_copy = pltpu.make_async_copy(tokens, tok, weight_sem.at[0])
    weight_copies = (
        pltpu.make_async_copy(gate_weight, gw, weight_sem.at[1]),
        pltpu.make_async_copy(up_weight, uw, weight_sem.at[2]),
    )
    for which in range(3):
        load(which, 0).start()
    token_copy.start()

    barrier = pltpu.get_barrier_semaphore()

    @pl.when(has_left)
    def _():
        pl.semaphore_signal(barrier, inc=1, device_id={"rep": z - 1}, device_id_type=MESH)

    @pl.when(has_right)
    def _():
        pl.semaphore_signal(barrier, inc=1, device_id={"rep": z + 1}, device_id_type=MESH)

    for d in range(1, tp_count):
        peer = lax.rem(me + d, tp_count)
        pl.semaphore_signal(barrier, inc=1, device_id={"tp": peer}, device_id_type=MESH)

    def start_load(b, carry):
        for which in range(3):
            load(which, b).start()
        return carry

    lax.fori_loop(1, blocks, start_load, 0)
    for copy in weight_copies:
        copy.start()

    zero_rows = jnp.zeros((PAD, CW), F32)
    gpad[0:PAD, :] = zero_rows
    upad[0:PAD, :] = zero_rows
    gdel[length : length + PAD, :] = zero_rows
    udel[length : length + PAD, :] = zero_rows

    tile = TILE if length % TILE == 0 else length
    piece_rows = length // 3 if length % (3 * tile) == 0 else length

    def folded(x):
        return jnp.sum(x.reshape(x.shape[0] // 8, 8, CW), axis=0)

    def elementwise(b, first_row, rows):
        cols = columns(b)
        gt = [gate_taps[k : k + 1, cols] for k in range(taps)]
        ut = [up_taps[k : k + 1, cols] for k in range(taps)]
        gb = gate_bias[cols].reshape(1, CW)
        ub = up_bias[cols].reshape(1, CW)

        def mix_back(r):
            gk = gdel[r + taps - 1 : r + taps - 1 + tile, :] * gt[0]
            uk = udel[r + taps - 1 : r + taps - 1 + tile, :] * ut[0]
            for k in range(1, taps):
                first = r + taps - 1 - k
                gk = gk + gdel[first : first + tile, :] * gt[k]
                uk = uk + udel[first : first + tile, :] * ut[k]
            gback[r : r + tile, :] = gk.astype(BF16)
            uback[r : r + tile, :] = uk.astype(BF16)

        sums = None
        for r in range(first_row, first_row + rows, tile):
            g_now = gpre[b, r : r + tile, :].astype(F32)
            u_now = upre[b, r : r + tile, :].astype(F32)
            gpad[PAD + r : PAD + r + tile, :] = g_now
            upad[PAD + r : PAD + r + tile, :] = u_now
            start = PAD + r - (taps - 1)
            gs = [gpad[start + k : start + k + tile, :] for k in range(taps - 1)] + [g_now]
            us = [upad[start + k : start + k + tile, :] for k in range(taps - 1)] + [u_now]
            gm = gs[0] * gt[0]
            um = us[0] * ut[0]
            for k in range(1, taps):
                gm = gm + gs[k] * gt[k]
                um = um + us[k] * ut[k]
            gm = gm + gb
            um = um + ub
            s = jax.nn.sigmoid(gm)
            hs = hid[b, r : r + tile, :].astype(F32) * s
            gd = hs * um * (1.0 + gm * (1.0 - s))
            ud = hs * gm
            gdel[r : r + tile, :] = gd
            udel[r : r + tile, :] = ud
            parts = (
                [folded(gd * g) for g in gs]
                + [folded(ud * u) for u in us]
                + [folded(gd), folded(ud)]
            )
            sums = parts if sums is None else [a + p for a, p in zip(sums, parts)]
            if r > 0:
                mix_back(r - tile)
        last = first_row + rows == length
        if last:
            mix_back(length - tile)
        for k, part in enumerate(sums):
            if first_row > 0:
                part = part + parts_ref[k]
            if last:
                small[k : k + 1, cols] = jnp.sum(part, axis=0, keepdims=True)
            else:
                parts_ref[k] = part

    def own_right(c):
        return pltpu.make_async_remote_copy(
            src_ref=own.at[c],
            dst_ref=from_left.at[c],
            send_sem=send_r.at[c],
            recv_sem=recv_r.at[c],
            device_id={"rep": z + 1},
            device_id_type=MESH,
        )

    def own_left(c):
        return pltpu.make_async_remote_copy(
            src_ref=own.at[c],
            dst_ref=from_right.at[c],
            send_sem=send_l.at[c],
            recv_sem=recv_l.at[c],
            device_id={"rep": z - 1},
            device_id_type=MESH,
        )

    def right_copy(c):
        return pltpu.make_async_remote_copy(
            src_ref=from_left.at[c],
            dst_ref=from_left.at[c],
            send_sem=send_r.at[c],
            recv_sem=recv_r.at[c],
            device_id={"rep": z + 1},
            device_id_type=MESH,
        )

    def left_copy(c):
        return pltpu.make_async_remote_copy(
            src_ref=to_left.at[c],
            dst_ref=from_right.at[c],
            send_sem=send_l.at[c],
            recv_sem=recv_l.at[c],
            device_id={"rep": z - 1},
            device_id_type=MESH,
        )

    def weight_grad(b, first, last):
        block = jnp.concatenate([gback[...], uback[...]], axis=1)
        for q in range(first, last):
            own[b * NQ + q] = jnp.dot(
                tok_t[q * rows_q : (q + 1) * rows_q, :], block, preferred_element_type=F32
            ).astype(BF16)

    def input_grad(b, fresh):
        cols = columns(b)
        weights = jnp.concatenate([gw[:, cols], uw[:, cols]], axis=1)
        dot_rows = 256 if length % 256 == 0 else length
        for r in range(0, length, dot_rows):
            value = lax.dot_general(
                jnp.concatenate([gback[r : r + dot_rows, :], uback[r : r + dot_rows, :]], axis=1),
                weights,
                (((1,), (1,)), ((), ())),
                preferred_element_type=F32,
            )
            if fresh:
                acc[r : r + dot_rows, :] = value
            else:
                acc[r : r + dot_rows, :] += value

    small_right = pltpu.make_async_remote_copy(
        src_ref=small_to_right,
        dst_ref=small_from_left,
        send_sem=small_sem.at[0],
        recv_sem=small_sem.at[1],
        device_id={"rep": z + 1},
        device_id_type=MESH,
    )
    small_left = pltpu.make_async_remote_copy(
        src_ref=small_to_left,
        dst_ref=small_from_right,
        send_sem=small_sem.at[2],
        recv_sem=small_sem.at[3],
        device_id={"rep": z - 1},
        device_id_type=MESH,
    )

    def scatter_copy(d):
        peer = lax.rem(me + d, tp_count)
        return pltpu.make_async_remote_copy(
            src_ref=term.at[peer],
            dst_ref=term_in.at[d - 1],
            send_sem=scatter_send.at[d - 1],
            recv_sem=scatter_recv.at[d - 1],
            device_id={"tp": peer},
            device_id_type=MESH,
        )

    def gather_copy(d, slot):
        return pltpu.make_async_remote_copy(
            src_ref=final.at[slot],
            dst_ref=final.at[slot],
            send_sem=gather_send.at[d - 1],
            recv_sem=gather_recv.at[d - 1],
            device_id={"tp": lax.rem(me + d, tp_count)},
            device_id_type=MESH,
        )

    term_rows = length // tp_count

    for which in range(3):
        load(which, 0).wait()
    elementwise(0, 0, length)
    token_copy.wait()
    per_turn = max(CW // rows_q, 1)
    early = min(per_turn, NQ)

    def turn(first, last):
        for i in range(first * rows_q, last * rows_q, CW):
            tok_t[i : i + CW, :] = tok[:, i : i + CW].T

    turn(0, early)
    pl.semaphore_wait(
        barrier,
        jnp.where(has_left, 1, 0) + jnp.where(has_right, 1, 0) + (tp_count - 1),
    )
    weight_grad(0, 0, early)
    if early < NQ:
        turn(early, NQ)
        weight_grad(0, early, NQ)
    for copy in weight_copies:
        copy.wait()
    input_grad(0, True)

    @pl.when(jnp.logical_not(has_left))
    def _():
        small_from_left[...] = jnp.zeros_like(small_from_left)

    @pl.when(jnp.logical_not(has_right))
    def _():
        small_from_right[...] = jnp.zeros_like(small_from_right)

    def move(tick):
        @pl.when(jnp.logical_not(has_left) & (tick < chunks))
        def _():
            own_right(tick).start()

        @pl.when(jnp.logical_not(has_right) & (tick < chunks))
        def _():
            own_left(tick).start()

        c_right = tick - LAG * z
        c_left = tick - LAG * (rep_count - 1 - z)
        c_out = tick - LAG * (rep_count - 1)

        @pl.when(has_left & (c_right >= 0) & (c_right < chunks))
        def _():
            c = c_right
            right_copy(c).wait_recv()

            @pl.when(has_right)
            def _():
                from_left[c] = (from_left[c].astype(F32) + own[c].astype(F32)).astype(BF16)
                right_copy(c).start()

        @pl.when(has_right & (c_left >= 0) & (c_left < chunks))
        def _():
            c = c_left
            left_copy(c).wait_recv()

            @pl.when(has_left)
            def _():
                to_left[c] = (from_right[c].astype(F32) + own[c].astype(F32)).astype(BF16)
                left_copy(c).start()

        @pl.when((c_out >= 0) & (c_out < chunks))
        def _():
            c = c_out

            @pl.when(both)
            def _():
                own[c] = (from_left[c].astype(F32) + from_right[c].astype(F32)).astype(BF16)

            @pl.when(jnp.logical_not(has_left))
            def _():
                own_right(c).wait_send()
                own[c] = (own[c].astype(F32) + from_right[c].astype(F32)).astype(BF16)

            @pl.when(jnp.logical_not(has_right))
            def _():
                own_left(c).wait_send()
                own[c] = (from_left[c].astype(F32) + own[c].astype(F32)).astype(BF16)

    def step(h, carry):
        b = h + 1
        for p in range(TICKS):
            move(h * TICKS + p)

            if p * piece_rows < length:

                @pl.when(b < blocks)
                def _():
                    if p == 0:
                        for which in range(3):
                            load(which, b).wait()
                    elementwise(b, p * piece_rows, piece_rows)

            elif p == TICKS - 1:

                @pl.when(b < blocks)
                def _():
                    weight_grad(b, 0, NQ)
                    input_grad(b, False)

        @pl.when(h == done)
        def _():
            for k in range(tp_count):
                term[k] = acc[k * term_rows : (k + 1) * term_rows, :].astype(BF16)
            for d in range(1, tp_count):
                scatter_copy(d).start()

        @pl.when(h == done + 4)
        def _():
            total = term[me].astype(F32)
            for d in range(1, tp_count):
                scatter_copy(d).wait()
                total = total + term_in[d - 1].astype(F32)
            final[me] = total.astype(BF16)
            for d in range(1, tp_count):
                gather_copy(d, me).start()

        @pl.when(h == done + z)
        def _():
            @pl.when(has_left)
            def _():
                small_right.wait_recv()

            @pl.when(has_right)
            def _():
                small_to_right[...] = small_from_left[...] + small[...]
                small_right.start()

        @pl.when(h == done + rep_count - 1 - z)
        def _():
            @pl.when(has_right)
            def _():
                small_left.wait_recv()

            @pl.when(has_left)
            def _():
                small_to_left[...] = small_from_right[...] + small[...]
                small_left.start()

        return carry

    lax.fori_loop(0, steps, step, 0)

    small_out[...] = small_from_left[...] + small[...] + small_from_right[...]
    for d in range(1, tp_count):
        gather_copy(d, lax.rem(me + tp_count - d, tp_count)).wait_recv()
    for d in range(1, tp_count):
        gather_copy(d, me).wait_send()

    @pl.when(has_right)
    def _():
        small_right.wait_send()

    @pl.when(has_left)
    def _():
        small_left.wait_send()

    @pl.when(both)
    def _():
        def drain(c, carry):
            right_copy(c).wait_send()
            left_copy(c).wait_send()
            return carry

        lax.fori_loop(0, chunks, drain, 0)


def spread(
    chunks_ref, final, small, grad_out, gate_out, up_out, gate_taps_out, up_taps_out,
    gate_bias_out, up_bias_out, gate_rows, up_rows, gate_small, up_small, gate_line,
    up_line, row_sem, grad_sem, small_sem,
):
    blocks = gate_out.shape[1] // CW
    rows_q = gate_out.shape[0] // NQ
    taps = gate_taps_out.shape[0]
    slots, term_rows = final.shape[0], final.shape[1]

    def rows_copy(which, q):
        return pltpu.make_async_copy(
            (gate_rows, up_rows)[which].at[q % 2],
            (gate_out, up_out)[which].at[q * rows_q : (q + 1) * rows_q, :],
            row_sem.at[which, q],
        )

    for q in range(NQ):
        if q >= 2:
            rows_copy(0, q - 2).wait()
            rows_copy(1, q - 2).wait()
        for b in range(blocks):
            chunk = chunks_ref[b * NQ + q]
            gate_rows[q % 2, :, b * CW : (b + 1) * CW] = chunk[:, 0:CW].astype(F32)
            up_rows[q % 2, :, b * CW : (b + 1) * CW] = chunk[:, CW : 2 * CW].astype(F32)
        rows_copy(0, q).start()
        rows_copy(1, q).start()

    gate_small[...] = small[0:taps, :]
    up_small[...] = small[taps : 2 * taps, :]
    gate_line[...] = small[2 * taps, :]
    up_line[...] = small[2 * taps + 1, :]
    copies = [
        pltpu.make_async_copy(
            final.at[k], grad_out.at[k * term_rows : (k + 1) * term_rows, :], grad_sem.at[k]
        )
        for k in range(slots)
    ] + [
        pltpu.make_async_copy(gate_small, gate_taps_out, small_sem.at[0]),
        pltpu.make_async_copy(up_small, up_taps_out, small_sem.at[1]),
        pltpu.make_async_copy(gate_line, gate_bias_out, small_sem.at[2]),
        pltpu.make_async_copy(up_line, up_bias_out, small_sem.at[3]),
    ]
    for copy in copies:
        copy.start()
    for copy in copies:
        copy.wait()
    for q in range(max(NQ - 2, 0), NQ):
        rows_copy(0, q).wait()
        rows_copy(1, q).wait()


def per_device(
    rep_count,
    tp_count,
    tokens,
    gate_pre,
    up_pre,
    hidden_grad,
    gate_weight,
    up_weight,
    gate_taps,
    up_taps,
    gate_bias,
    up_bias,
):
    length, hidden_cols = gate_pre.shape
    width = tokens.shape[1]
    taps = gate_taps.shape[0]
    blocks = hidden_cols // CW
    chunks = blocks * NQ
    rows_q = width // NQ
    term_rows = length // tp_count
    small_rows = 2 * taps + 2
    anywhere = pl.BlockSpec(memory_space=pl.ANY)
    vmem = pl.BlockSpec(memory_space=pltpu.VMEM)
    line = pltpu.VMEM((chunks, rows_q, 2 * CW), BF16)
    small = pltpu.VMEM((small_rows, hidden_cols), F32)
    dma = pltpu.SemaphoreType.DMA
    summed, final, small_sum = pl.pallas_call(
        functools.partial(fused, rep_count, tp_count),
        out_shape=(
            pltpu.VMEM((chunks, rows_q, 2 * CW), BF16),
            pltpu.VMEM((tp_count, term_rows, width), BF16),
            pltpu.VMEM((small_rows, hidden_cols), F32),
        ),
        in_specs=[anywhere] * 6 + [vmem] * 4,
        out_specs=(vmem, vmem, vmem),
        scratch_shapes=[
            pltpu.VMEM((length, width), BF16),
            pltpu.VMEM((width, length), BF16),
            pltpu.VMEM((blocks, length, CW), BF16),
            pltpu.VMEM((blocks, length, CW), BF16),
            pltpu.VMEM((blocks, length, CW), BF16),
            pltpu.VMEM((width, hidden_cols), BF16),
            pltpu.VMEM((width, hidden_cols), BF16),
            pltpu.VMEM((PAD + length, CW), F32),
            pltpu.VMEM((PAD + length, CW), F32),
            pltpu.VMEM((length + PAD, CW), F32),
            pltpu.VMEM((length + PAD, CW), F32),
            pltpu.VMEM((length, CW), BF16),
            pltpu.VMEM((length, CW), BF16),
            pltpu.VMEM((small_rows, 8, CW), F32),
            pltpu.VMEM((length, width), F32),
            line,
            line,
            line,
            pltpu.VMEM((tp_count, term_rows, width), BF16),
            pltpu.VMEM((tp_count - 1, term_rows, width), BF16),
            small,
            small,
            small,
            small,
            small,
            dma((3, blocks)),
            dma((3,)),
            dma((chunks,)),
            dma((chunks,)),
            dma((chunks,)),
            dma((chunks,)),
            dma((tp_count - 1,)),
            dma((tp_count - 1,)),
            dma((tp_count - 1,)),
            dma((tp_count - 1,)),
            dma((4,)),
        ],
        compiler_params=pltpu.CompilerParams(
            collective_id=0, has_side_effects=True, vmem_limit_bytes=48 * 2**20
        ),
    )(
        tokens,
        gate_pre,
        up_pre,
        hidden_grad,
        gate_weight,
        up_weight,
        gate_taps,
        up_taps,
        gate_bias,
        up_bias,
    )
    held = [pltpu.with_memory_space_constraint(x, pltpu.VMEM) for x in (summed, final, small_sum)]
    return pl.pallas_call(
        spread,
        out_shape=(
            jax.ShapeDtypeStruct((length, width), BF16),
            jax.ShapeDtypeStruct((width, hidden_cols), F32),
            jax.ShapeDtypeStruct((width, hidden_cols), F32),
            jax.ShapeDtypeStruct((taps, hidden_cols), F32),
            jax.ShapeDtypeStruct((taps, hidden_cols), F32),
            jax.ShapeDtypeStruct((hidden_cols,), F32),
            jax.ShapeDtypeStruct((hidden_cols,), F32),
        ),
        in_specs=[vmem] * 3,
        out_specs=[anywhere] * 7,
        scratch_shapes=[
            pltpu.VMEM((2, rows_q, hidden_cols), F32),
            pltpu.VMEM((2, rows_q, hidden_cols), F32),
            pltpu.VMEM((taps, hidden_cols), F32),
            pltpu.VMEM((taps, hidden_cols), F32),
            pltpu.VMEM((hidden_cols,), F32),
            pltpu.VMEM((hidden_cols,), F32),
            dma((2, NQ)),
            dma((tp_count,)),
            dma((4,)),
        ],
        compiler_params=pltpu.CompilerParams(vmem_limit_bytes=8 * 2**20),
    )(*held)


def solution(mesh):
    return jax.shard_map(
        functools.partial(per_device, mesh.shape["rep"], mesh.shape["tp"]),
        mesh=mesh,
        in_specs=(
            P("rep", "fs"),
            P("rep", "tp"),
            P("rep", "tp"),
            P("rep", "tp"),
            P("fs", "tp"),
            P("fs", "tp"),
            P(None, "tp"),
            P(None, "tp"),
            P("tp"),
            P("tp"),
        ),
        out_specs=(
            P("rep", "fs"),
            P("fs", "tp"),
            P("fs", "tp"),
            P(None, "tp"),
            P(None, "tp"),
            P("tp"),
            P("tp"),
        ),
        check_vma=False,
    )
```

```python
import functools

import jax
import jax.numpy as jnp
from jax import lax
from jax.experimental import pallas as pl
from jax.experimental.pallas import tpu as pltpu
from jax.sharding import PartitionSpec as P

MESH = pl.DeviceIdType.MESH
CW = 128
NQ = 8
PAD = 8
TICKS = 4
LAG = 4
WINDOW = 2
SLOTS = 3
TILE = 32
F32 = jnp.float32
BF16 = jnp.bfloat16


def schedule(blocks, rep_count):
    done = max(blocks - 1, 0)
    last_tick = blocks * NQ + LAG * (rep_count - 1)
    steps = max(-(-last_tick // TICKS), done + rep_count, done + 5)
    return done, steps


def fused(
    rep_count,
    tp_count,
    tokens,
    gate_pre,
    up_pre,
    hidden,
    gate_weight,
    up_weight,
    gate_taps_hbm,
    up_taps_hbm,
    gate_bias_hbm,
    up_bias_hbm,
    own,
    final,
    small_out,
    tok,
    tok_t,
    gpre,
    upre,
    hid,
    gw,
    uw,
    gpad,
    upad,
    gdel,
    udel,
    gback,
    uback,
    parts_ref,
    acc,
    from_left,
    from_right,
    to_left,
    term,
    term_in,
    gate_taps,
    up_taps,
    gate_bias,
    up_bias,
    small,
    small_from_left,
    small_from_right,
    small_to_right,
    small_to_left,
    load_sem,
    weight_sem,
    send_r,
    recv_r,
    send_l,
    recv_l,
    scatter_send,
    scatter_recv,
    gather_send,
    gather_recv,
    small_sem,
):
    z = lax.axis_index("rep")
    me = lax.axis_index("tp")
    length, hidden_cols = gate_pre.shape
    width = tokens.shape[1]
    blocks = hidden_cols // CW
    chunks = blocks * NQ
    rows_q = width // NQ
    taps = gate_taps.shape[0]
    done, steps = schedule(blocks, rep_count)
    ring = recv_r.shape[0]
    has_left = z > 0
    has_right = z < rep_count - 1
    both = has_left & has_right

    def columns(b):
        return pl.ds(pl.multiple_of(b * CW, CW), CW)

    def load(which, b):
        src = (gate_pre, up_pre, hidden)[which]
        dst = (gpre, upre, hid)[which]
        return pltpu.make_async_copy(
            src.at[:, columns(b)], dst.at[b], load_sem.at[which, lax.rem(b, SLOTS)]
        )

    token_copy = pltpu.make_async_copy(tokens, tok, weight_sem.at[0])
    weight_copies = (
        pltpu.make_async_copy(gate_weight, gw, weight_sem.at[1]),
        pltpu.make_async_copy(up_weight, uw, weight_sem.at[2]),
    )
    small_copies = [
        pltpu.make_async_copy(src, dst, weight_sem.at[3 + i])
        for i, (src, dst) in enumerate(
            (
                (gate_taps_hbm, gate_taps),
                (up_taps_hbm, up_taps),
                (gate_bias_hbm, gate_bias),
                (up_bias_hbm, up_bias),
            )
        )
    ]
    for which in range(3):
        load(which, 0).start()
    for copy in small_copies:
        copy.start()
    token_copy.start()

    barrier = pltpu.get_barrier_semaphore()

    @pl.when(has_left)
    def _():
        pl.semaphore_signal(barrier, inc=1, device_id={"rep": z - 1}, device_id_type=MESH)

    @pl.when(has_right)
    def _():
        pl.semaphore_signal(barrier, inc=1, device_id={"rep": z + 1}, device_id_type=MESH)

    for d in range(1, tp_count):
        peer = lax.rem(me + d, tp_count)
        pl.semaphore_signal(barrier, inc=1, device_id={"tp": peer}, device_id_type=MESH)

    def start_load(b, carry):
        for which in range(3):
            load(which, b).start()
        return carry

    for b in range(1, min(SLOTS, blocks)):
        start_load(b, 0)
    for copy in weight_copies:
        copy.start()

    zero_rows = jnp.zeros((PAD, CW), F32)
    gpad[0:PAD, :] = zero_rows
    upad[0:PAD, :] = zero_rows
    gdel[length : length + PAD, :] = zero_rows
    udel[length : length + PAD, :] = zero_rows

    tile = TILE if length % TILE == 0 else length
    piece_rows = length // 3 if length % (3 * tile) == 0 else length

    def folded(x):
        return jnp.sum(x.reshape(x.shape[0] // 8, 8, CW), axis=0)

    def elementwise(b, first_row, rows):
        cols = columns(b)
        gt = [gate_taps[k : k + 1, cols] for k in range(taps)]
        ut = [up_taps[k : k + 1, cols] for k in range(taps)]
        gb = gate_bias[cols].reshape(1, CW)
        ub = up_bias[cols].reshape(1, CW)

        def mix_back(r):
            gk = gdel[r + taps - 1 : r + taps - 1 + tile, :] * gt[0]
            uk = udel[r + taps - 1 : r + taps - 1 + tile, :] * ut[0]
            for k in range(1, taps):
                first = r + taps - 1 - k
                gk = gk + gdel[first : first + tile, :] * gt[k]
                uk = uk + udel[first : first + tile, :] * ut[k]
            gback[r : r + tile, :] = gk.astype(BF16)
            uback[r : r + tile, :] = uk.astype(BF16)

        sums = None
        for r in range(first_row, first_row + rows, tile):
            g_now = gpre[b, r : r + tile, :].astype(F32)
            u_now = upre[b, r : r + tile, :].astype(F32)
            gpad[PAD + r : PAD + r + tile, :] = g_now
            upad[PAD + r : PAD + r + tile, :] = u_now
            start = PAD + r - (taps - 1)
            gs = [gpad[start + k : start + k + tile, :] for k in range(taps - 1)] + [g_now]
            us = [upad[start + k : start + k + tile, :] for k in range(taps - 1)] + [u_now]
            gm = gs[0] * gt[0]
            um = us[0] * ut[0]
            for k in range(1, taps):
                gm = gm + gs[k] * gt[k]
                um = um + us[k] * ut[k]
            gm = gm + gb
            um = um + ub
            s = jax.nn.sigmoid(gm)
            hs = hid[b, r : r + tile, :].astype(F32) * s
            gd = hs * um * (1.0 + gm * (1.0 - s))
            ud = hs * gm
            gdel[r : r + tile, :] = gd
            udel[r : r + tile, :] = ud
            parts = (
                [folded(gd * g) for g in gs]
                + [folded(ud * u) for u in us]
                + [folded(gd), folded(ud)]
            )
            sums = parts if sums is None else [a + p for a, p in zip(sums, parts)]
            if r > 0:
                mix_back(r - tile)
        last = first_row + rows == length
        if last:
            mix_back(length - tile)
        for k, part in enumerate(sums):
            if first_row > 0:
                part = part + parts_ref[k]
            if last:
                small[k : k + 1, cols] = jnp.sum(part, axis=0, keepdims=True)
            else:
                parts_ref[k] = part

    def own_right(c):
        return pltpu.make_async_remote_copy(
            src_ref=own.at[c],
            dst_ref=from_left.at[c],
            send_sem=send_r.at[lax.rem(c, WINDOW)],
            recv_sem=recv_r.at[lax.rem(c, ring)],
            device_id={"rep": z + 1},
            device_id_type=MESH,
        )

    def own_left(c):
        return pltpu.make_async_remote_copy(
            src_ref=own.at[c],
            dst_ref=from_right.at[c],
            send_sem=send_l.at[lax.rem(c, WINDOW)],
            recv_sem=recv_l.at[lax.rem(c, ring)],
            device_id={"rep": z - 1},
            device_id_type=MESH,
        )

    def right_copy(c):
        return pltpu.make_async_remote_copy(
            src_ref=from_left.at[c],
            dst_ref=from_left.at[c],
            send_sem=send_r.at[lax.rem(c, WINDOW)],
            recv_sem=recv_r.at[lax.rem(c, ring)],
            device_id={"rep": z + 1},
            device_id_type=MESH,
        )

    def left_copy(c):
        return pltpu.make_async_remote_copy(
            src_ref=to_left.at[c],
            dst_ref=from_right.at[c],
            send_sem=send_l.at[lax.rem(c, WINDOW)],
            recv_sem=recv_l.at[lax.rem(c, ring)],
            device_id={"rep": z - 1},
            device_id_type=MESH,
        )

    def weight_grad(b, first, last):
        block = jnp.concatenate([gback[...], uback[...]], axis=1)
        for q in range(first, last):
            own[b * NQ + q] = jnp.dot(
                tok_t[q * rows_q : (q + 1) * rows_q, :], block, preferred_element_type=F32
            ).astype(BF16)

    def input_grad(b, fresh):
        cols = columns(b)
        weights = jnp.concatenate([gw[:, cols], uw[:, cols]], axis=1)
        dot_rows = 256 if length % 256 == 0 else length
        for r in range(0, length, dot_rows):
            value = lax.dot_general(
                jnp.concatenate([gback[r : r + dot_rows, :], uback[r : r + dot_rows, :]], axis=1),
                weights,
                (((1,), (1,)), ((), ())),
                preferred_element_type=F32,
            )
            if fresh:
                acc[r : r + dot_rows, :] = value
            else:
                acc[r : r + dot_rows, :] += value

    small_right = pltpu.make_async_remote_copy(
        src_ref=small_to_right,
        dst_ref=small_from_left,
        send_sem=small_sem.at[0],
        recv_sem=small_sem.at[1],
        device_id={"rep": z + 1},
        device_id_type=MESH,
    )
    small_left = pltpu.make_async_remote_copy(
        src_ref=small_to_left,
        dst_ref=small_from_right,
        send_sem=small_sem.at[2],
        recv_sem=small_sem.at[3],
        device_id={"rep": z - 1},
        device_id_type=MESH,
    )

    def scatter_copy(d):
        peer = lax.rem(me + d, tp_count)
        return pltpu.make_async_remote_copy(
            src_ref=term.at[peer],
            dst_ref=term_in.at[d - 1],
            send_sem=scatter_send.at[d - 1],
            recv_sem=scatter_recv.at[d - 1],
            device_id={"tp": peer},
            device_id_type=MESH,
        )

    def gather_copy(d, slot):
        return pltpu.make_async_remote_copy(
            src_ref=final.at[slot],
            dst_ref=final.at[slot],
            send_sem=gather_send.at[d - 1],
            recv_sem=gather_recv.at[d - 1],
            device_id={"tp": lax.rem(me + d, tp_count)},
            device_id_type=MESH,
        )

    term_rows = length // tp_count

    for which in range(3):
        load(which, 0).wait()
    for copy in small_copies:
        copy.wait()
    elementwise(0, 0, length)
    token_copy.wait()
    per_turn = max(CW // rows_q, 1)
    early = min(per_turn, NQ)

    def turn(first, last):
        for i in range(first * rows_q, last * rows_q, CW):
            tok_t[i : i + CW, :] = tok[:, i : i + CW].T

    turn(0, early)
    pl.semaphore_wait(
        barrier,
        jnp.where(has_left, 1, 0) + jnp.where(has_right, 1, 0) + (tp_count - 1),
    )
    weight_grad(0, 0, early)
    if early < NQ:
        turn(early, NQ)
        weight_grad(0, early, NQ)
    for copy in weight_copies:
        copy.wait()
    input_grad(0, True)

    @pl.when(jnp.logical_not(has_left))
    def _():
        small_from_left[...] = jnp.zeros_like(small_from_left)

    @pl.when(jnp.logical_not(has_right))
    def _():
        small_from_right[...] = jnp.zeros_like(small_from_right)

    def move(tick):
        c_right = tick - LAG * z
        c_left = tick - LAG * (rep_count - 1 - z)
        c_out = tick - LAG * (rep_count - 1)

        @pl.when(has_right & (c_right >= WINDOW) & (c_right < chunks + WINDOW))
        def _():
            right_copy(c_right - WINDOW).wait_send()

        @pl.when((c_right >= 0) & (c_right < chunks))
        def _():
            c = c_right

            @pl.when(jnp.logical_not(has_left))
            def _():
                own_right(c).start()

            @pl.when(has_left)
            def _():
                right_copy(c).wait_recv()

            @pl.when(both)
            def _():
                from_left[c] = (from_left[c].astype(F32) + own[c].astype(F32)).astype(BF16)
                right_copy(c).start()

        @pl.when(has_left & (c_left >= WINDOW) & (c_left < chunks + WINDOW))
        def _():
            left_copy(c_left - WINDOW).wait_send()

        @pl.when((c_left >= 0) & (c_left < chunks))
        def _():
            c = c_left

            @pl.when(jnp.logical_not(has_right))
            def _():
                own_left(c).start()

            @pl.when(has_right)
            def _():
                left_copy(c).wait_recv()

            @pl.when(both)
            def _():
                to_left[c] = (from_right[c].astype(F32) + own[c].astype(F32)).astype(BF16)
                left_copy(c).start()

        @pl.when((c_out >= 0) & (c_out < chunks))
        def _():
            c = c_out

            @pl.when(both)
            def _():
                own[c] = (from_left[c].astype(F32) + from_right[c].astype(F32)).astype(BF16)

            @pl.when(jnp.logical_not(has_left))
            def _():
                own[c] = (own[c].astype(F32) + from_right[c].astype(F32)).astype(BF16)

            @pl.when(jnp.logical_not(has_right))
            def _():
                own[c] = (from_left[c].astype(F32) + own[c].astype(F32)).astype(BF16)

    def step(h, carry):
        b = h + 1
        for p in range(TICKS):
            move(h * TICKS + p)

            if p * piece_rows < length:

                @pl.when(b < blocks)
                def _():
                    if p == 0:
                        for which in range(3):
                            load(which, b).wait()

                        @pl.when(b + SLOTS - 1 < blocks)
                        def _():
                            start_load(b + SLOTS - 1, 0)

                    elementwise(b, p * piece_rows, piece_rows)

            elif p == TICKS - 1:

                @pl.when(b < blocks)
                def _():
                    weight_grad(b, 0, NQ)
                    input_grad(b, False)

        @pl.when(h == done)
        def _():
            for k in range(tp_count):
                term[k] = acc[k * term_rows : (k + 1) * term_rows, :].astype(BF16)
            for d in range(1, tp_count):
                scatter_copy(d).start()

        @pl.when(h == done + 4)
        def _():
            total = term[me].astype(F32)
            for d in range(1, tp_count):
                scatter_copy(d).wait()
                total = total + term_in[d - 1].astype(F32)
            final[me] = total.astype(BF16)
            for d in range(1, tp_count):
                gather_copy(d, me).start()

        @pl.when(h == done + z)
        def _():
            @pl.when(has_left)
            def _():
                small_right.wait_recv()

            @pl.when(has_right)
            def _():
                small_to_right[...] = (small_from_left[...].astype(F32) + small[...]).astype(BF16)
                small_right.start()

        @pl.when(h == done + rep_count - 1 - z)
        def _():
            @pl.when(has_right)
            def _():
                small_left.wait_recv()

            @pl.when(has_left)
            def _():
                small_to_left[...] = (small_from_right[...].astype(F32) + small[...]).astype(BF16)
                small_left.start()

        return carry

    lax.fori_loop(0, steps, step, 0)

    small_out[...] = small_from_left[...].astype(F32) + small[...] + small_from_right[...].astype(F32)
    for d in range(1, tp_count):
        gather_copy(d, lax.rem(me + tp_count - d, tp_count)).wait_recv()
    for d in range(1, tp_count):
        gather_copy(d, me).wait_send()

    @pl.when(has_right)
    def _():
        small_right.wait_send()

    @pl.when(has_left)
    def _():
        small_left.wait_send()


def spread(
    chunks_ref, final, small, grad_out, gate_out, up_out, gate_taps_out, up_taps_out,
    gate_bias_out, up_bias_out, gate_rows, up_rows, gate_small, up_small, gate_line,
    up_line, row_sem, grad_sem, small_sem,
):
    blocks = gate_out.shape[1] // CW
    rows_q = gate_out.shape[0] // NQ
    taps = gate_taps_out.shape[0]
    slots, term_rows = final.shape[0], final.shape[1]

    def rows_copy(which, q):
        return pltpu.make_async_copy(
            (gate_rows, up_rows)[which].at[q],
            (gate_out, up_out)[which].at[q * rows_q : (q + 1) * rows_q, :],
            row_sem.at[which, q],
        )

    gate_small[...] = small[0:taps, :]
    up_small[...] = small[taps : 2 * taps, :]
    gate_line[...] = small[2 * taps, :]
    up_line[...] = small[2 * taps + 1, :]
    copies = [
        pltpu.make_async_copy(
            final.at[k], grad_out.at[k * term_rows : (k + 1) * term_rows, :], grad_sem.at[k]
        )
        for k in range(slots)
    ] + [
        pltpu.make_async_copy(gate_small, gate_taps_out, small_sem.at[0]),
        pltpu.make_async_copy(up_small, up_taps_out, small_sem.at[1]),
        pltpu.make_async_copy(gate_line, gate_bias_out, small_sem.at[2]),
        pltpu.make_async_copy(up_line, up_bias_out, small_sem.at[3]),
    ]
    for copy in copies:
        copy.start()
    for q in range(NQ):
        for b in range(blocks):
            chunk = chunks_ref[b * NQ + q]
            gate_rows[q, :, b * CW : (b + 1) * CW] = chunk[:, 0:CW].astype(F32)
            up_rows[q, :, b * CW : (b + 1) * CW] = chunk[:, CW : 2 * CW].astype(F32)
        rows_copy(0, q).start()
        rows_copy(1, q).start()
    for copy in copies:
        copy.wait()
    for q in range(NQ):
        rows_copy(0, q).wait()
        rows_copy(1, q).wait()


def per_device(
    rep_count,
    tp_count,
    tokens,
    gate_pre,
    up_pre,
    hidden_grad,
    gate_weight,
    up_weight,
    gate_taps,
    up_taps,
    gate_bias,
    up_bias,
):
    length, hidden_cols = gate_pre.shape
    width = tokens.shape[1]
    taps = gate_taps.shape[0]
    blocks = hidden_cols // CW
    chunks = blocks * NQ
    rows_q = width // NQ
    term_rows = length // tp_count
    ring = min(chunks, LAG * (rep_count - 1) + TICKS)
    small_rows = 2 * taps + 2
    anywhere = pl.BlockSpec(memory_space=pl.ANY)
    vmem = pl.BlockSpec(memory_space=pltpu.VMEM)
    line = pltpu.VMEM((chunks, rows_q, 2 * CW), BF16)
    small = pltpu.VMEM((small_rows, hidden_cols), F32)
    small_line = pltpu.VMEM((small_rows, hidden_cols), BF16)
    dma = pltpu.SemaphoreType.DMA
    summed, final, small_sum = pl.pallas_call(
        functools.partial(fused, rep_count, tp_count),
        out_shape=(
            pltpu.VMEM((chunks, rows_q, 2 * CW), BF16),
            pltpu.VMEM((tp_count, term_rows, width), BF16),
            pltpu.VMEM((small_rows, hidden_cols), F32),
        ),
        in_specs=[anywhere] * 10,
        out_specs=(vmem, vmem, vmem),
        scratch_shapes=[
            pltpu.VMEM((length, width), BF16),
            pltpu.VMEM((width, length), BF16),
            pltpu.VMEM((blocks, length, CW), BF16),
            pltpu.VMEM((blocks, length, CW), BF16),
            pltpu.VMEM((blocks, length, CW), BF16),
            pltpu.VMEM((width, hidden_cols), BF16),
            pltpu.VMEM((width, hidden_cols), BF16),
            pltpu.VMEM((PAD + length, CW), F32),
            pltpu.VMEM((PAD + length, CW), F32),
            pltpu.VMEM((length + PAD, CW), F32),
            pltpu.VMEM((length + PAD, CW), F32),
            pltpu.VMEM((length, CW), BF16),
            pltpu.VMEM((length, CW), BF16),
            pltpu.VMEM((small_rows, 8, CW), F32),
            pltpu.VMEM((length, width), F32),
            line,
            line,
            line,
            pltpu.VMEM((tp_count, term_rows, width), BF16),
            pltpu.VMEM((tp_count - 1, term_rows, width), BF16),
            pltpu.VMEM((taps, hidden_cols), F32),
            pltpu.VMEM((taps, hidden_cols), F32),
            pltpu.VMEM((hidden_cols,), F32),
            pltpu.VMEM((hidden_cols,), F32),
            small,
            small_line,
            small_line,
            small_line,
            small_line,
            dma((3, SLOTS)),
            dma((7,)),
            dma((WINDOW,)),
            dma((ring,)),
            dma((WINDOW,)),
            dma((ring,)),
            dma((tp_count - 1,)),
            dma((tp_count - 1,)),
            dma((tp_count - 1,)),
            dma((tp_count - 1,)),
            dma((4,)),
        ],
        compiler_params=pltpu.CompilerParams(
            collective_id=0, has_side_effects=True, vmem_limit_bytes=48 * 2**20
        ),
    )(
        tokens,
        gate_pre,
        up_pre,
        hidden_grad,
        gate_weight,
        up_weight,
        gate_taps,
        up_taps,
        gate_bias,
        up_bias,
    )
    held = [pltpu.with_memory_space_constraint(x, pltpu.VMEM) for x in (summed, final, small_sum)]
    return pl.pallas_call(
        spread,
        out_shape=(
            jax.ShapeDtypeStruct((length, width), BF16),
            jax.ShapeDtypeStruct((width, hidden_cols), F32),
            jax.ShapeDtypeStruct((width, hidden_cols), F32),
            jax.ShapeDtypeStruct((taps, hidden_cols), F32),
            jax.ShapeDtypeStruct((taps, hidden_cols), F32),
            jax.ShapeDtypeStruct((hidden_cols,), F32),
            jax.ShapeDtypeStruct((hidden_cols,), F32),
        ),
        in_specs=[vmem] * 3,
        out_specs=[anywhere] * 7,
        scratch_shapes=[
            pltpu.VMEM((NQ, rows_q, hidden_cols), F32),
            pltpu.VMEM((NQ, rows_q, hidden_cols), F32),
            pltpu.VMEM((taps, hidden_cols), F32),
            pltpu.VMEM((taps, hidden_cols), F32),
            pltpu.VMEM((hidden_cols,), F32),
            pltpu.VMEM((hidden_cols,), F32),
            dma((2, NQ)),
            dma((tp_count,)),
            dma((4,)),
        ],
        compiler_params=pltpu.CompilerParams(vmem_limit_bytes=16 * 2**20),
    )(*held)


def solution(mesh):
    return jax.shard_map(
        functools.partial(per_device, mesh.shape["rep"], mesh.shape["tp"]),
        mesh=mesh,
        in_specs=(
            P("rep", "fs"),
            P("rep", "tp"),
            P("rep", "tp"),
            P("rep", "tp"),
            P("fs", "tp"),
            P("fs", "tp"),
            P(None, "tp"),
            P(None, "tp"),
            P("tp"),
            P("tp"),
        ),
        out_specs=(
            P("rep", "fs"),
            P("fs", "tp"),
            P("fs", "tp"),
            P(None, "tp"),
            P(None, "tp"),
            P("tp"),
            P("tp"),
        ),
        check_vma=False,
    )
```

```python
import functools

import jax
import jax.numpy as jnp
from jax import lax
from jax.experimental import pallas as pl
from jax.experimental.pallas import tpu as pltpu
from jax.sharding import PartitionSpec as P

MESH = pl.DeviceIdType.MESH
CW = 128
NQ = 8
PAD = 8
TICKS = NQ // 2
PIECE = TICKS // 4
LAG = 3
WINDOW = 3
SLOTS = 3
TILE = 32
F32 = jnp.float32
BF16 = jnp.bfloat16


def schedule(blocks, rep_count):
    done = blocks
    last_tick = blocks * NQ + LAG * (rep_count - 1)
    steps = max(-(-(last_tick - 1) // TICKS), done + 2 * rep_count, done + rep_count + 4)
    return done, steps


def fused(
    rep_count,
    tp_count,
    tokens,
    gate_pre,
    up_pre,
    hidden,
    gate_weight,
    up_weight,
    gate_taps_hbm,
    up_taps_hbm,
    gate_bias_hbm,
    up_bias_hbm,
    own,
    final,
    small_out,
    tok,
    tok_t,
    gpre,
    upre,
    hid,
    gw,
    uw,
    gpad,
    upad,
    gdel,
    udel,
    gback,
    uback,
    parts_ref,
    acc,
    from_left,
    from_right,
    to_left,
    term,
    term_in,
    gate_taps,
    up_taps,
    gate_bias,
    up_bias,
    small,
    small_from_left,
    small_from_right,
    small_to_right,
    small_to_left,
    load_sem,
    weight_sem,
    send_r,
    recv_r,
    send_l,
    recv_l,
    scatter_send,
    scatter_recv,
    gather_send,
    gather_recv,
    small_sem,
):
    z = lax.axis_index("rep")
    me = lax.axis_index("tp")
    length, hidden_cols = gate_pre.shape
    width = tokens.shape[1]
    blocks = hidden_cols // CW
    chunks = blocks * NQ
    rows_q = width // NQ
    taps = gate_taps.shape[0]
    done, steps = schedule(blocks, rep_count)
    ring = recv_r.shape[0]
    has_left = z > 0
    has_right = z < rep_count - 1
    both = has_left & has_right

    barrier = pltpu.get_barrier_semaphore()

    @pl.when(has_left)
    def _():
        pl.semaphore_signal(barrier, inc=1, device_id={"rep": z - 1}, device_id_type=MESH)

    @pl.when(has_right)
    def _():
        pl.semaphore_signal(barrier, inc=1, device_id={"rep": z + 1}, device_id_type=MESH)

    for d in range(1, tp_count):
        peer = lax.rem(me + d, tp_count)
        pl.semaphore_signal(barrier, inc=1, device_id={"tp": peer}, device_id_type=MESH)

    def columns(b):
        return pl.ds(pl.multiple_of(b * CW, CW), CW)

    def load(which, b):
        src = (gate_pre, up_pre, hidden)[which]
        dst = (gpre, upre, hid)[which]
        return pltpu.make_async_copy(
            src.at[:, columns(b)], dst.at[b], load_sem.at[which, lax.rem(b, SLOTS)]
        )

    token_copies = [
        pltpu.make_async_copy(tokens.at[:, part], tok.at[:, part], weight_sem.at[i])
        for i, part in ((0, pl.ds(0, CW)), (7, pl.ds(CW, width - CW)))
    ]
    weight_copies = (
        pltpu.make_async_copy(gate_weight, gw, weight_sem.at[1]),
        pltpu.make_async_copy(up_weight, uw, weight_sem.at[2]),
    )
    small_copies = [
        pltpu.make_async_copy(src, dst, weight_sem.at[3 + i])
        for i, (src, dst) in enumerate(
            (
                (gate_taps_hbm, gate_taps),
                (up_taps_hbm, up_taps),
                (gate_bias_hbm, gate_bias),
                (up_bias_hbm, up_bias),
            )
        )
    ]
    for which in range(3):
        load(which, 0).start()
    for copy in small_copies:
        copy.start()
    for copy in token_copies:
        copy.start()

    def start_load(b, carry):
        for which in range(3):
            load(which, b).start()
        return carry

    zero_rows = jnp.zeros((PAD, CW), F32)
    gpad[0:PAD, :] = zero_rows
    upad[0:PAD, :] = zero_rows
    gdel[length : length + PAD, :] = zero_rows
    udel[length : length + PAD, :] = zero_rows

    tile = TILE if length % TILE == 0 else length

    def folded(x):
        return jnp.sum(x.reshape(x.shape[0] // 8, 8, CW), axis=0)

    def elementwise(b, first_row, rows):
        cols = columns(b)
        gt = [gate_taps[k : k + 1, cols] for k in range(taps)]
        ut = [up_taps[k : k + 1, cols] for k in range(taps)]
        gb = gate_bias[cols].reshape(1, CW)
        ub = up_bias[cols].reshape(1, CW)

        def mix_back(r):
            gk = gdel[r + taps - 1 : r + taps - 1 + tile, :] * gt[0]
            uk = udel[r + taps - 1 : r + taps - 1 + tile, :] * ut[0]
            for k in range(1, taps):
                first = r + taps - 1 - k
                gk = gk + gdel[first : first + tile, :] * gt[k]
                uk = uk + udel[first : first + tile, :] * ut[k]
            gback[r : r + tile, :] = gk.astype(BF16)
            uback[r : r + tile, :] = uk.astype(BF16)

        sums = None
        for r in range(first_row, first_row + rows, tile):
            g_now = gpre[b, r : r + tile, :].astype(F32)
            u_now = upre[b, r : r + tile, :].astype(F32)
            gpad[PAD + r : PAD + r + tile, :] = g_now
            upad[PAD + r : PAD + r + tile, :] = u_now
            start = PAD + r - (taps - 1)
            gs = [gpad[start + k : start + k + tile, :] for k in range(taps - 1)] + [g_now]
            us = [upad[start + k : start + k + tile, :] for k in range(taps - 1)] + [u_now]
            gm = gs[0] * gt[0]
            um = us[0] * ut[0]
            for k in range(1, taps):
                gm = gm + gs[k] * gt[k]
                um = um + us[k] * ut[k]
            gm = gm + gb
            um = um + ub
            s = jax.nn.sigmoid(gm)
            hs = hid[b, r : r + tile, :].astype(F32) * s
            gd = hs * um * (1.0 + gm * (1.0 - s))
            ud = hs * gm
            gdel[r : r + tile, :] = gd
            udel[r : r + tile, :] = ud
            parts = (
                [folded(gd * g) for g in gs]
                + [folded(ud * u) for u in us]
                + [folded(gd), folded(ud)]
            )
            sums = parts if sums is None else [a + p for a, p in zip(sums, parts)]
            if r > 0:
                mix_back(r - tile)
        last = first_row + rows == length
        if last:
            mix_back(length - tile)
        for k, part in enumerate(sums):
            if first_row > 0:
                part = part + parts_ref[k]
            if last:
                small[k : k + 1, cols] = jnp.sum(part, axis=0, keepdims=True)
            else:
                parts_ref[k] = part

    def own_right(c):
        return pltpu.make_async_remote_copy(
            src_ref=own.at[c],
            dst_ref=from_left.at[c],
            send_sem=send_r.at[lax.rem(c, WINDOW)],
            recv_sem=recv_r.at[lax.rem(c, ring)],
            device_id={"rep": z + 1},
            device_id_type=MESH,
        )

    def own_left(c):
        return pltpu.make_async_remote_copy(
            src_ref=own.at[c],
            dst_ref=from_right.at[c],
            send_sem=send_l.at[lax.rem(c, WINDOW)],
            recv_sem=recv_l.at[lax.rem(c, ring)],
            device_id={"rep": z - 1},
            device_id_type=MESH,
        )

    def right_copy(c):
        return pltpu.make_async_remote_copy(
            src_ref=from_left.at[c],
            dst_ref=from_left.at[c],
            send_sem=send_r.at[lax.rem(c, WINDOW)],
            recv_sem=recv_r.at[lax.rem(c, ring)],
            device_id={"rep": z + 1},
            device_id_type=MESH,
        )

    def left_copy(c):
        return pltpu.make_async_remote_copy(
            src_ref=to_left.at[c],
            dst_ref=from_right.at[c],
            send_sem=send_l.at[lax.rem(c, WINDOW)],
            recv_sem=recv_l.at[lax.rem(c, ring)],
            device_id={"rep": z - 1},
            device_id_type=MESH,
        )

    def weight_grad(b, first, last):
        block = jnp.concatenate([gback[...], uback[...]], axis=1)
        for q in range(first, last):
            own[b * NQ + q] = jnp.dot(
                tok_t[q * rows_q : (q + 1) * rows_q, :], block, preferred_element_type=F32
            ).astype(BF16)

    dot_rows = 256 if length % 256 == 0 else length

    def input_grad(b, fresh, begin, end):
        cols = columns(b)
        weights = jnp.concatenate([gw[:, cols], uw[:, cols]], axis=1)
        for r in range(begin, end, dot_rows):
            value = lax.dot_general(
                jnp.concatenate([gback[r : r + dot_rows, :], uback[r : r + dot_rows, :]], axis=1),
                weights,
                (((1,), (1,)), ((), ())),
                preferred_element_type=F32,
            )
            if fresh:
                acc[r : r + dot_rows, :] = value
            else:
                acc[r : r + dot_rows, :] += value

    small_right = pltpu.make_async_remote_copy(
        src_ref=small_to_right,
        dst_ref=small_from_left,
        send_sem=small_sem.at[0],
        recv_sem=small_sem.at[1],
        device_id={"rep": z + 1},
        device_id_type=MESH,
    )
    small_left = pltpu.make_async_remote_copy(
        src_ref=small_to_left,
        dst_ref=small_from_right,
        send_sem=small_sem.at[2],
        recv_sem=small_sem.at[3],
        device_id={"rep": z - 1},
        device_id_type=MESH,
    )

    def scatter_copy(d):
        peer = lax.rem(me + d, tp_count)
        return pltpu.make_async_remote_copy(
            src_ref=term.at[peer],
            dst_ref=term_in.at[d - 1],
            send_sem=scatter_send.at[d - 1],
            recv_sem=scatter_recv.at[d - 1],
            device_id={"tp": peer},
            device_id_type=MESH,
        )

    def gather_copy(d, slot):
        return pltpu.make_async_remote_copy(
            src_ref=final.at[slot],
            dst_ref=final.at[slot],
            send_sem=gather_send.at[d - 1],
            recv_sem=gather_recv.at[d - 1],
            device_id={"tp": lax.rem(me + d, tp_count)},
            device_id_type=MESH,
        )

    term_rows = length // tp_count

    def move(tick):
        c_right = tick - LAG * z
        c_left = tick - LAG * (rep_count - 1 - z)
        c_out = tick - LAG * (rep_count - 1)

        @pl.when(has_left & (c_left >= WINDOW) & (c_left < chunks + WINDOW))
        def _():
            left_copy(c_left - WINDOW).wait_send()

        @pl.when((c_left >= 0) & (c_left < chunks))
        def _():
            c = c_left

            @pl.when(jnp.logical_not(has_right))
            def _():
                own_left(c).start()

            @pl.when(has_right)
            def _():
                left_copy(c).wait_recv()

            @pl.when(both)
            def _():
                to_left[c] = (from_right[c].astype(F32) + own[c].astype(F32)).astype(BF16)
                left_copy(c).start()

        @pl.when(has_right & (c_right >= WINDOW) & (c_right < chunks + WINDOW))
        def _():
            right_copy(c_right - WINDOW).wait_send()

        @pl.when((c_right >= 0) & (c_right < chunks))
        def _():
            c = c_right

            @pl.when(jnp.logical_not(has_left))
            def _():
                own_right(c).start()

            @pl.when(has_left)
            def _():
                right_copy(c).wait_recv()

            @pl.when(both)
            def _():
                from_left[c] = (from_left[c].astype(F32) + own[c].astype(F32)).astype(BF16)
                right_copy(c).start()

        @pl.when((c_out >= 0) & (c_out < chunks))
        def _():
            c = c_out

            @pl.when(both)
            def _():
                own[c] = (from_left[c].astype(F32) + from_right[c].astype(F32)).astype(BF16)

            @pl.when(jnp.logical_not(has_left))
            def _():
                own[c] = (own[c].astype(F32) + from_right[c].astype(F32)).astype(BF16)

            @pl.when(jnp.logical_not(has_right))
            def _():
                own[c] = (from_left[c].astype(F32) + own[c].astype(F32)).astype(BF16)

    for which in range(3):
        load(which, 0).wait()
    for copy in small_copies:
        copy.wait()
    elementwise(0, 0, length)
    per_turn = max(CW // rows_q, 1)
    early = min(per_turn, NQ)

    def turn(first, last):
        for i in range(first * rows_q, last * rows_q, CW):
            tok_t[i : i + CW, :] = tok[:, i : i + CW].T

    token_copies[0].wait()
    turn(0, early)
    weight_grad(0, 0, early)
    pl.semaphore_wait(
        barrier,
        jnp.where(has_left, 1, 0) + jnp.where(has_right, 1, 0) + (tp_count - 1),
    )
    move(0)
    token_copies[1].wait()
    for b in range(1, min(SLOTS, blocks)):
        start_load(b, 0)
    for copy in weight_copies:
        copy.start()
    if early < NQ:
        turn(early, NQ)
        weight_grad(0, early, NQ)

    @pl.when(jnp.logical_not(has_left))
    def _():
        small_from_left[...] = jnp.zeros_like(small_from_left)

    @pl.when(jnp.logical_not(has_right))
    def _():
        small_from_right[...] = jnp.zeros_like(small_from_right)

    def step(h, carry):
        b = h
        for p in range(TICKS):
            move(h * TICKS + p + 1)

            if p == TICKS // 2:

                @pl.when(h == 0)
                def _():
                    for copy in weight_copies:
                        copy.wait()
                    input_grad(0, True, 0, length)


            @pl.when((b > 0) & (b < blocks))
            def _():
                if p == 0:
                    for which in range(3):
                        load(which, b).wait()

                    @pl.when(b + SLOTS - 1 < blocks)
                    def _():
                        start_load(b + SLOTS - 1, 0)

                    elementwise(b, 0, length)
                elif p == PIECE:
                    weight_grad(b, 0, NQ)
                elif p == 2 * PIECE:
                    input_grad(b, False, 0, dot_rows * (length // dot_rows * 2 // 3))
                elif p == 3 * PIECE:
                    input_grad(b, False, dot_rows * (length // dot_rows * 2 // 3), length)

        @pl.when(h == done)
        def _():
            for k in range(tp_count):
                term[k] = acc[k * term_rows : (k + 1) * term_rows, :].astype(BF16)
            for d in range(1, tp_count):
                scatter_copy(d).start()

        @pl.when(h == done + 4)
        def _():
            total = term[me].astype(F32)
            for d in range(1, tp_count):
                scatter_copy(d).wait()
                total = total + term_in[d - 1].astype(F32)
            final[me] = total.astype(BF16)
            for d in range(1, tp_count):
                gather_copy(d, me).start()

        @pl.when(h == done + z)
        def _():
            @pl.when(has_left)
            def _():
                small_right.wait_recv()

            @pl.when(has_right)
            def _():
                small_to_right[...] = (small_from_left[...].astype(F32) + small[...]).astype(BF16)
                small_right.start()

        @pl.when(h == done + rep_count - 1 - z)
        def _():
            @pl.when(has_right)
            def _():
                small_left.wait_recv()

            @pl.when(has_left)
            def _():
                small_to_left[...] = (small_from_right[...].astype(F32) + small[...]).astype(BF16)
                small_left.start()

        @pl.when(h == steps - 1 - (rep_count - 2))
        def _():
            small_out[...] = (
                small_from_left[...].astype(F32) + small[...] + small_from_right[...].astype(F32)
            )
            for d in range(1, tp_count):
                gather_copy(d, lax.rem(me + tp_count - d, tp_count)).wait_recv()
            for d in range(1, tp_count):
                gather_copy(d, me).wait_send()

            @pl.when(has_right)
            def _():
                small_right.wait_send()

            @pl.when(has_left)
            def _():
                small_left.wait_send()

        return carry

    lax.fori_loop(0, steps, step, 0)


def spread(
    chunks_ref, final, small, grad_out, gate_out, up_out, gate_taps_out, up_taps_out,
    gate_bias_out, up_bias_out, gate_rows, up_rows, gate_small, up_small, gate_line,
    up_line, row_sem, grad_sem, small_sem,
):
    blocks = gate_out.shape[1] // CW
    rows_q = gate_out.shape[0] // NQ
    taps = gate_taps_out.shape[0]
    slots, term_rows = final.shape[0], final.shape[1]

    def rows_copy(which, q):
        return pltpu.make_async_copy(
            (gate_rows, up_rows)[which].at[q],
            (gate_out, up_out)[which].at[q * rows_q : (q + 1) * rows_q, :],
            row_sem.at[which, q],
        )

    gate_small[...] = small[0:taps, :]
    up_small[...] = small[taps : 2 * taps, :]
    gate_line[...] = small[2 * taps, :]
    up_line[...] = small[2 * taps + 1, :]
    copies = [
        pltpu.make_async_copy(
            final.at[k], grad_out.at[k * term_rows : (k + 1) * term_rows, :], grad_sem.at[k]
        )
        for k in range(slots)
    ] + [
        pltpu.make_async_copy(gate_small, gate_taps_out, small_sem.at[0]),
        pltpu.make_async_copy(up_small, up_taps_out, small_sem.at[1]),
        pltpu.make_async_copy(gate_line, gate_bias_out, small_sem.at[2]),
        pltpu.make_async_copy(up_line, up_bias_out, small_sem.at[3]),
    ]
    for copy in copies:
        copy.start()
    for q in range(NQ):
        for b in range(blocks):
            chunk = chunks_ref[b * NQ + q]
            gate_rows[q, :, b * CW : (b + 1) * CW] = chunk[:, 0:CW].astype(F32)
            up_rows[q, :, b * CW : (b + 1) * CW] = chunk[:, CW : 2 * CW].astype(F32)
        rows_copy(0, q).start()
        rows_copy(1, q).start()
    for copy in copies:
        copy.wait()
    for q in range(NQ):
        rows_copy(0, q).wait()
        rows_copy(1, q).wait()


def per_device(
    rep_count,
    tp_count,
    tokens,
    gate_pre,
    up_pre,
    hidden_grad,
    gate_weight,
    up_weight,
    gate_taps,
    up_taps,
    gate_bias,
    up_bias,
):
    length, hidden_cols = gate_pre.shape
    width = tokens.shape[1]
    taps = gate_taps.shape[0]
    blocks = hidden_cols // CW
    chunks = blocks * NQ
    rows_q = width // NQ
    term_rows = length // tp_count
    ring = min(chunks, LAG * (rep_count - 1) + TICKS)
    small_rows = 2 * taps + 2
    anywhere = pl.BlockSpec(memory_space=pl.ANY)
    vmem = pl.BlockSpec(memory_space=pltpu.VMEM)
    line = pltpu.VMEM((chunks, rows_q, 2 * CW), BF16)
    small = pltpu.VMEM((small_rows, hidden_cols), F32)
    small_line = pltpu.VMEM((small_rows, hidden_cols), BF16)
    dma = pltpu.SemaphoreType.DMA
    summed, final, small_sum = pl.pallas_call(
        functools.partial(fused, rep_count, tp_count),
        out_shape=(
            pltpu.VMEM((chunks, rows_q, 2 * CW), BF16),
            pltpu.VMEM((tp_count, term_rows, width), BF16),
            pltpu.VMEM((small_rows, hidden_cols), F32),
        ),
        in_specs=[anywhere] * 10,
        out_specs=(vmem, vmem, vmem),
        scratch_shapes=[
            pltpu.VMEM((length, width), BF16),
            pltpu.VMEM((width, length), BF16),
            pltpu.VMEM((blocks, length, CW), BF16),
            pltpu.VMEM((blocks, length, CW), BF16),
            pltpu.VMEM((blocks, length, CW), BF16),
            pltpu.VMEM((width, hidden_cols), BF16),
            pltpu.VMEM((width, hidden_cols), BF16),
            pltpu.VMEM((PAD + length, CW), F32),
            pltpu.VMEM((PAD + length, CW), F32),
            pltpu.VMEM((length + PAD, CW), F32),
            pltpu.VMEM((length + PAD, CW), F32),
            pltpu.VMEM((length, CW), BF16),
            pltpu.VMEM((length, CW), BF16),
            pltpu.VMEM((small_rows, 8, CW), F32),
            pltpu.VMEM((length, width), F32),
            line,
            line,
            line,
            pltpu.VMEM((tp_count, term_rows, width), BF16),
            pltpu.VMEM((tp_count - 1, term_rows, width), BF16),
            pltpu.VMEM((taps, hidden_cols), F32),
            pltpu.VMEM((taps, hidden_cols), F32),
            pltpu.VMEM((hidden_cols,), F32),
            pltpu.VMEM((hidden_cols,), F32),
            small,
            small_line,
            small_line,
            small_line,
            small_line,
            dma((3, SLOTS)),
            dma((8,)),
            dma((WINDOW,)),
            dma((ring,)),
            dma((WINDOW,)),
            dma((ring,)),
            dma((tp_count - 1,)),
            dma((tp_count - 1,)),
            dma((tp_count - 1,)),
            dma((tp_count - 1,)),
            dma((4,)),
        ],
        compiler_params=pltpu.CompilerParams(
            collective_id=0, has_side_effects=True, vmem_limit_bytes=48 * 2**20
        ),
    )(
        tokens,
        gate_pre,
        up_pre,
        hidden_grad,
        gate_weight,
        up_weight,
        gate_taps,
        up_taps,
        gate_bias,
        up_bias,
    )
    held = [pltpu.with_memory_space_constraint(x, pltpu.VMEM) for x in (summed, final, small_sum)]
    return pl.pallas_call(
        spread,
        out_shape=(
            jax.ShapeDtypeStruct((length, width), BF16),
            jax.ShapeDtypeStruct((width, hidden_cols), F32),
            jax.ShapeDtypeStruct((width, hidden_cols), F32),
            jax.ShapeDtypeStruct((taps, hidden_cols), F32),
            jax.ShapeDtypeStruct((taps, hidden_cols), F32),
            jax.ShapeDtypeStruct((hidden_cols,), F32),
            jax.ShapeDtypeStruct((hidden_cols,), F32),
        ),
        in_specs=[vmem] * 3,
        out_specs=[anywhere] * 7,
        scratch_shapes=[
            pltpu.VMEM((NQ, rows_q, hidden_cols), F32),
            pltpu.VMEM((NQ, rows_q, hidden_cols), F32),
            pltpu.VMEM((taps, hidden_cols), F32),
            pltpu.VMEM((taps, hidden_cols), F32),
            pltpu.VMEM((hidden_cols,), F32),
            pltpu.VMEM((hidden_cols,), F32),
            dma((2, NQ)),
            dma((tp_count,)),
            dma((4,)),
        ],
        compiler_params=pltpu.CompilerParams(vmem_limit_bytes=16 * 2**20),
    )(*held)


def solution(mesh):
    return jax.shard_map(
        functools.partial(per_device, mesh.shape["rep"], mesh.shape["tp"]),
        mesh=mesh,
        in_specs=(
            P("rep", "fs"),
            P("rep", "tp"),
            P("rep", "tp"),
            P("rep", "tp"),
            P("fs", "tp"),
            P("fs", "tp"),
            P(None, "tp"),
            P(None, "tp"),
            P("tp"),
            P("tp"),
        ),
        out_specs=(
            P("rep", "fs"),
            P("fs", "tp"),
            P("fs", "tp"),
            P(None, "tp"),
            P(None, "tp"),
            P("tp"),
            P("tp"),
        ),
        check_vma=False,
    )
```

```python
import functools

import jax
import jax.numpy as jnp
from jax import lax
from jax.experimental import pallas as pl
from jax.experimental.pallas import tpu as pltpu
from jax.sharding import PartitionSpec as P

MESH = pl.DeviceIdType.MESH
CW = 128
NQ = 16
PAD = 8
TICKS = NQ // 2
PIECE = TICKS // 4
LAG_LEFT = 6
LAG_RIGHT = 6
WINDOW = 5
SLOTS = 3
TILE = 32
F32 = jnp.float32
BF16 = jnp.bfloat16


def schedule(blocks, rep_count):
    done = blocks
    last_tick = blocks * NQ + LAG_RIGHT * (rep_count - 1)
    steps = max(-(-(last_tick - 1) // TICKS), done + 2 * rep_count, done + rep_count + 6)
    return done, steps


def fused(
    rep_count,
    tp_count,
    tokens,
    gate_pre,
    up_pre,
    hidden,
    gate_weight,
    up_weight,
    gate_taps_hbm,
    up_taps_hbm,
    gate_bias_hbm,
    up_bias_hbm,
    own,
    final,
    small_out,
    tok,
    tok_t,
    gpre,
    upre,
    hid,
    gw,
    uw,
    gpad,
    upad,
    gdel,
    udel,
    gback,
    uback,
    parts_ref,
    acc,
    from_left,
    from_right,
    to_left,
    term,
    term_in,
    gate_taps,
    up_taps,
    gate_bias,
    up_bias,
    small,
    small_from_left,
    small_from_right,
    small_to_right,
    small_to_left,
    load_sem,
    weight_sem,
    send_r,
    recv_r,
    send_l,
    recv_l,
    scatter_send,
    scatter_recv,
    gather_send,
    gather_recv,
    small_sem,
):
    z = lax.axis_index("rep")
    me = lax.axis_index("tp")
    length, hidden_cols = gate_pre.shape
    width = tokens.shape[1]
    blocks = hidden_cols // CW
    chunks = blocks * NQ
    rows_q = width // NQ
    taps = gate_taps.shape[0]
    done, steps = schedule(blocks, rep_count)
    ring = recv_r.shape[0]
    has_left = z > 0
    has_right = z < rep_count - 1
    both = has_left & has_right

    barrier = pltpu.get_barrier_semaphore()

    @pl.when(has_left)
    def _():
        pl.semaphore_signal(barrier, inc=1, device_id={"rep": z - 1}, device_id_type=MESH)

    @pl.when(has_right)
    def _():
        pl.semaphore_signal(barrier, inc=1, device_id={"rep": z + 1}, device_id_type=MESH)

    for d in range(1, tp_count):
        peer = lax.rem(me + d, tp_count)
        pl.semaphore_signal(barrier, inc=1, device_id={"tp": peer}, device_id_type=MESH)

    def columns(b):
        return pl.ds(pl.multiple_of(b * CW, CW), CW)

    def load(which, b):
        src = (gate_pre, up_pre, hidden)[which]
        dst = (gpre, upre, hid)[which]
        return pltpu.make_async_copy(
            src.at[:, columns(b)], dst.at[b], load_sem.at[which, lax.rem(b, SLOTS)]
        )

    token_copies = [
        pltpu.make_async_copy(tokens.at[:, part], tok.at[:, part], weight_sem.at[i])
        for i, part in ((0, pl.ds(0, CW)), (7, pl.ds(CW, width - CW)))
    ]
    weight_copies = (
        pltpu.make_async_copy(gate_weight, gw, weight_sem.at[1]),
        pltpu.make_async_copy(up_weight, uw, weight_sem.at[2]),
    )
    small_copies = [
        pltpu.make_async_copy(src, dst, weight_sem.at[3 + i])
        for i, (src, dst) in enumerate(
            (
                (gate_taps_hbm, gate_taps),
                (up_taps_hbm, up_taps),
                (gate_bias_hbm, gate_bias),
                (up_bias_hbm, up_bias),
            )
        )
    ]
    for which in range(3):
        load(which, 0).start()
    for copy in small_copies:
        copy.start()
    for copy in token_copies:
        copy.start()

    def start_load(b, carry):
        for which in range(3):
            load(which, b).start()
        return carry

    zero_rows = jnp.zeros((PAD, CW), F32)
    gpad[0:PAD, :] = zero_rows
    upad[0:PAD, :] = zero_rows
    gdel[length : length + PAD, :] = zero_rows
    udel[length : length + PAD, :] = zero_rows

    tile = TILE if length % TILE == 0 else length

    def folded(x):
        return jnp.sum(x.reshape(x.shape[0] // 8, 8, CW), axis=0)

    def elementwise(b, first_row, rows):
        cols = columns(b)
        gt = [gate_taps[k : k + 1, cols] for k in range(taps)]
        ut = [up_taps[k : k + 1, cols] for k in range(taps)]
        gb = gate_bias[cols].reshape(1, CW)
        ub = up_bias[cols].reshape(1, CW)

        def mix_back(r):
            gk = gdel[r + taps - 1 : r + taps - 1 + tile, :] * gt[0]
            uk = udel[r + taps - 1 : r + taps - 1 + tile, :] * ut[0]
            for k in range(1, taps):
                first = r + taps - 1 - k
                gk = gk + gdel[first : first + tile, :] * gt[k]
                uk = uk + udel[first : first + tile, :] * ut[k]
            gback[r : r + tile, :] = gk.astype(BF16)
            uback[r : r + tile, :] = uk.astype(BF16)

        sums = None
        for r in range(first_row, first_row + rows, tile):
            g_now = gpre[b, r : r + tile, :].astype(F32)
            u_now = upre[b, r : r + tile, :].astype(F32)
            gpad[PAD + r : PAD + r + tile, :] = g_now
            upad[PAD + r : PAD + r + tile, :] = u_now
            start = PAD + r - (taps - 1)
            gs = [gpad[start + k : start + k + tile, :] for k in range(taps - 1)] + [g_now]
            us = [upad[start + k : start + k + tile, :] for k in range(taps - 1)] + [u_now]
            gm = gs[0] * gt[0]
            um = us[0] * ut[0]
            for k in range(1, taps):
                gm = gm + gs[k] * gt[k]
                um = um + us[k] * ut[k]
            gm = gm + gb
            um = um + ub
            s = jax.nn.sigmoid(gm)
            hs = hid[b, r : r + tile, :].astype(F32) * s
            gd = hs * um * (1.0 + gm * (1.0 - s))
            ud = hs * gm
            gdel[r : r + tile, :] = gd
            udel[r : r + tile, :] = ud
            parts = (
                [folded(gd * g) for g in gs]
                + [folded(ud * u) for u in us]
                + [folded(gd), folded(ud)]
            )
            sums = parts if sums is None else [a + p for a, p in zip(sums, parts)]
            if r > 0:
                mix_back(r - tile)
        last = first_row + rows == length
        if last:
            mix_back(length - tile)
        for k, part in enumerate(sums):
            if first_row > 0:
                part = part + parts_ref[k]
            if last:
                small[k : k + 1, cols] = jnp.sum(part, axis=0, keepdims=True)
            else:
                parts_ref[k] = part

    def own_right(c):
        return pltpu.make_async_remote_copy(
            src_ref=own.at[c],
            dst_ref=from_left.at[c],
            send_sem=send_r.at[lax.rem(c, WINDOW)],
            recv_sem=recv_r.at[lax.rem(c, ring)],
            device_id={"rep": z + 1},
            device_id_type=MESH,
        )

    def own_left(c):
        return pltpu.make_async_remote_copy(
            src_ref=own.at[c],
            dst_ref=from_right.at[c],
            send_sem=send_l.at[lax.rem(c, WINDOW)],
            recv_sem=recv_l.at[lax.rem(c, ring)],
            device_id={"rep": z - 1},
            device_id_type=MESH,
        )

    def right_copy(c):
        return pltpu.make_async_remote_copy(
            src_ref=from_left.at[c],
            dst_ref=from_left.at[c],
            send_sem=send_r.at[lax.rem(c, WINDOW)],
            recv_sem=recv_r.at[lax.rem(c, ring)],
            device_id={"rep": z + 1},
            device_id_type=MESH,
        )

    def left_copy(c):
        return pltpu.make_async_remote_copy(
            src_ref=to_left.at[c],
            dst_ref=from_right.at[c],
            send_sem=send_l.at[lax.rem(c, WINDOW)],
            recv_sem=recv_l.at[lax.rem(c, ring)],
            device_id={"rep": z - 1},
            device_id_type=MESH,
        )

    def weight_grad(b, first, last):
        block = jnp.concatenate([gback[...], uback[...]], axis=1)
        for q in range(first, last):
            own[b * NQ + q] = jnp.dot(
                tok_t[q * rows_q : (q + 1) * rows_q, :], block, preferred_element_type=F32
            ).astype(BF16)

    dot_rows = 256 if length % 256 == 0 else length

    def input_grad(b, fresh, begin, end):
        cols = columns(b)
        weights = jnp.concatenate([gw[:, cols], uw[:, cols]], axis=1)
        for r in range(begin, end, dot_rows):
            value = lax.dot_general(
                jnp.concatenate([gback[r : r + dot_rows, :], uback[r : r + dot_rows, :]], axis=1),
                weights,
                (((1,), (1,)), ((), ())),
                preferred_element_type=F32,
            )
            if fresh:
                acc[r : r + dot_rows, :] = value
            else:
                acc[r : r + dot_rows, :] += value

    small_right = pltpu.make_async_remote_copy(
        src_ref=small_to_right,
        dst_ref=small_from_left,
        send_sem=small_sem.at[0],
        recv_sem=small_sem.at[1],
        device_id={"rep": z + 1},
        device_id_type=MESH,
    )
    small_left = pltpu.make_async_remote_copy(
        src_ref=small_to_left,
        dst_ref=small_from_right,
        send_sem=small_sem.at[2],
        recv_sem=small_sem.at[3],
        device_id={"rep": z - 1},
        device_id_type=MESH,
    )

    def scatter_copy(d):
        peer = lax.rem(me + d, tp_count)
        return pltpu.make_async_remote_copy(
            src_ref=term.at[peer],
            dst_ref=term_in.at[d - 1],
            send_sem=scatter_send.at[d - 1],
            recv_sem=scatter_recv.at[d - 1],
            device_id={"tp": peer},
            device_id_type=MESH,
        )

    def gather_copy(d, slot):
        return pltpu.make_async_remote_copy(
            src_ref=final.at[slot],
            dst_ref=final.at[slot],
            send_sem=gather_send.at[d - 1],
            recv_sem=gather_recv.at[d - 1],
            device_id={"tp": lax.rem(me + d, tp_count)},
            device_id_type=MESH,
        )

    term_rows = length // tp_count

    def move(tick):
        c_right = tick - LAG_RIGHT * z
        c_left = tick - LAG_LEFT * (rep_count - 1 - z)
        c_out = jnp.minimum(c_right, c_left)

        @pl.when(has_left & (c_left >= WINDOW) & (c_left < chunks + WINDOW))
        def _():
            left_copy(c_left - WINDOW).wait_send()

        @pl.when((c_left >= 0) & (c_left < chunks))
        def _():
            c = c_left

            @pl.when(jnp.logical_not(has_right))
            def _():
                own_left(c).start()

            @pl.when(has_right)
            def _():
                left_copy(c).wait_recv()

            @pl.when(both)
            def _():
                to_left[c] = (from_right[c].astype(F32) + own[c].astype(F32)).astype(BF16)
                left_copy(c).start()

        @pl.when(has_right & (c_right >= WINDOW) & (c_right < chunks + WINDOW))
        def _():
            right_copy(c_right - WINDOW).wait_send()

        @pl.when((c_right >= 0) & (c_right < chunks))
        def _():
            c = c_right

            @pl.when(jnp.logical_not(has_left))
            def _():
                own_right(c).start()

            @pl.when(has_left)
            def _():
                right_copy(c).wait_recv()

            @pl.when(both)
            def _():
                from_left[c] = (from_left[c].astype(F32) + own[c].astype(F32)).astype(BF16)
                right_copy(c).start()

        @pl.when((c_out >= 0) & (c_out < chunks))
        def _():
            c = c_out

            @pl.when(both)
            def _():
                own[c] = (from_left[c].astype(F32) + from_right[c].astype(F32)).astype(BF16)

            @pl.when(jnp.logical_not(has_left))
            def _():
                own[c] = (own[c].astype(F32) + from_right[c].astype(F32)).astype(BF16)

            @pl.when(jnp.logical_not(has_right))
            def _():
                own[c] = (from_left[c].astype(F32) + own[c].astype(F32)).astype(BF16)

    for which in range(3):
        load(which, 0).wait()
    for copy in small_copies:
        copy.wait()
    elementwise(0, 0, length)
    per_turn = max(CW // rows_q, 1)
    early = min(per_turn, NQ)

    def turn(first, last):
        for i in range(first * rows_q, last * rows_q, CW):
            tok_t[i : i + CW, :] = tok[:, i : i + CW].T

    token_copies[0].wait()
    turn(0, early)
    weight_grad(0, 0, early)
    pl.semaphore_wait(
        barrier,
        jnp.where(has_left, 1, 0) + jnp.where(has_right, 1, 0) + (tp_count - 1),
    )
    move(0)
    token_copies[1].wait()
    for b in range(1, min(SLOTS, blocks)):
        start_load(b, 0)
    for copy in weight_copies:
        copy.start()
    if early < NQ:
        turn(early, NQ)
        weight_grad(0, early, NQ)

    @pl.when(jnp.logical_not(has_left))
    def _():
        small_from_left[...] = jnp.zeros_like(small_from_left)

    @pl.when(jnp.logical_not(has_right))
    def _():
        small_from_right[...] = jnp.zeros_like(small_from_right)

    def step(h, carry):
        b = h
        for p in range(TICKS):
            move(h * TICKS + p + 1)

            @pl.when(h == done)
            def _():
                for k in range(p, tp_count, TICKS):
                    term[k] = acc[k * term_rows : (k + 1) * term_rows, :].astype(BF16)
                if p == TICKS - 1:
                    for d in range(1, tp_count):
                        scatter_copy(d).start()

            if p == TICKS // 2:

                @pl.when(h == 0)
                def _():
                    for copy in weight_copies:
                        copy.wait()
                    input_grad(0, True, 0, length)


            @pl.when((b > 0) & (b < blocks))
            def _():
                if p == 0:
                    for which in range(3):
                        load(which, b).wait()

                    @pl.when(b + SLOTS - 1 < blocks)
                    def _():
                        start_load(b + SLOTS - 1, 0)

                    elementwise(b, 0, length)
                elif p == PIECE:
                    weight_grad(b, 0, NQ)
                elif p == 2 * PIECE:
                    input_grad(b, False, 0, dot_rows * (length // dot_rows * 2 // 3))
                elif p == 3 * PIECE:
                    input_grad(b, False, dot_rows * (length // dot_rows * 2 // 3), length)

        @pl.when(h == done + 5)
        def _():
            total = term[me].astype(F32)
            for d in range(1, tp_count):
                scatter_copy(d).wait()
                total = total + term_in[d - 1].astype(F32)
            final[me] = total.astype(BF16)
            for d in range(1, tp_count):
                gather_copy(d, me).start()

        @pl.when(h == done + z)
        def _():
            @pl.when(has_left)
            def _():
                small_right.wait_recv()

            @pl.when(has_right)
            def _():
                small_to_right[...] = (small_from_left[...].astype(F32) + small[...]).astype(BF16)
                small_right.start()

        @pl.when(h == done + rep_count - 1 - z)
        def _():
            @pl.when(has_right)
            def _():
                small_left.wait_recv()

            @pl.when(has_left)
            def _():
                small_to_left[...] = (small_from_right[...].astype(F32) + small[...]).astype(BF16)
                small_left.start()

        @pl.when(h == steps - 1 - (rep_count - 2))
        def _():
            small_out[...] = (
                small_from_left[...].astype(F32) + small[...] + small_from_right[...].astype(F32)
            )
            for d in range(1, tp_count):
                gather_copy(d, lax.rem(me + tp_count - d, tp_count)).wait_recv()
            for d in range(1, tp_count):
                gather_copy(d, me).wait_send()

            @pl.when(has_right)
            def _():
                small_right.wait_send()

            @pl.when(has_left)
            def _():
                small_left.wait_send()

        return carry

    lax.fori_loop(0, steps, step, 0)


def spread(
    chunks_ref, final, small, grad_out, gate_out, up_out, gate_taps_out, up_taps_out,
    gate_bias_out, up_bias_out, gate_rows, up_rows, gate_small, up_small, gate_line,
    up_line, row_sem, grad_sem, small_sem,
):
    blocks = gate_out.shape[1] // CW
    rows_q = gate_out.shape[0] // NQ
    taps = gate_taps_out.shape[0]
    slots, term_rows = final.shape[0], final.shape[1]

    def rows_copy(which, q):
        return pltpu.make_async_copy(
            (gate_rows, up_rows)[which].at[q],
            (gate_out, up_out)[which].at[q * rows_q : (q + 1) * rows_q, :],
            row_sem.at[which, q],
        )

    gate_small[...] = small[0:taps, :]
    up_small[...] = small[taps : 2 * taps, :]
    gate_line[...] = small[2 * taps, :]
    up_line[...] = small[2 * taps + 1, :]
    copies = [
        pltpu.make_async_copy(
            final.at[k], grad_out.at[k * term_rows : (k + 1) * term_rows, :], grad_sem.at[k]
        )
        for k in range(slots)
    ] + [
        pltpu.make_async_copy(gate_small, gate_taps_out, small_sem.at[0]),
        pltpu.make_async_copy(up_small, up_taps_out, small_sem.at[1]),
        pltpu.make_async_copy(gate_line, gate_bias_out, small_sem.at[2]),
        pltpu.make_async_copy(up_line, up_bias_out, small_sem.at[3]),
    ]
    for copy in copies:
        copy.start()
    for q in range(NQ):
        for b in range(blocks):
            chunk = chunks_ref[b * NQ + q]
            gate_rows[q, :, b * CW : (b + 1) * CW] = chunk[:, 0:CW].astype(F32)
            up_rows[q, :, b * CW : (b + 1) * CW] = chunk[:, CW : 2 * CW].astype(F32)
        rows_copy(0, q).start()
        rows_copy(1, q).start()
    for copy in copies:
        copy.wait()
    for q in range(NQ):
        rows_copy(0, q).wait()
        rows_copy(1, q).wait()


def per_device(
    rep_count,
    tp_count,
    tokens,
    gate_pre,
    up_pre,
    hidden_grad,
    gate_weight,
    up_weight,
    gate_taps,
    up_taps,
    gate_bias,
    up_bias,
):
    length, hidden_cols = gate_pre.shape
    width = tokens.shape[1]
    taps = gate_taps.shape[0]
    blocks = hidden_cols // CW
    chunks = blocks * NQ
    rows_q = width // NQ
    term_rows = length // tp_count
    ring = min(chunks, LAG_RIGHT * (rep_count - 1) + TICKS)
    small_rows = 2 * taps + 2
    anywhere = pl.BlockSpec(memory_space=pl.ANY)
    vmem = pl.BlockSpec(memory_space=pltpu.VMEM)
    line = pltpu.VMEM((chunks, rows_q, 2 * CW), BF16)
    small = pltpu.VMEM((small_rows, hidden_cols), F32)
    small_line = pltpu.VMEM((small_rows, hidden_cols), BF16)
    dma = pltpu.SemaphoreType.DMA
    summed, final, small_sum = pl.pallas_call(
        functools.partial(fused, rep_count, tp_count),
        out_shape=(
            pltpu.VMEM((chunks, rows_q, 2 * CW), BF16),
            pltpu.VMEM((tp_count, term_rows, width), BF16),
            pltpu.VMEM((small_rows, hidden_cols), F32),
        ),
        in_specs=[anywhere] * 10,
        out_specs=(vmem, vmem, vmem),
        scratch_shapes=[
            pltpu.VMEM((length, width), BF16),
            pltpu.VMEM((width, length), BF16),
            pltpu.VMEM((blocks, length, CW), BF16),
            pltpu.VMEM((blocks, length, CW), BF16),
            pltpu.VMEM((blocks, length, CW), BF16),
            pltpu.VMEM((width, hidden_cols), BF16),
            pltpu.VMEM((width, hidden_cols), BF16),
            pltpu.VMEM((PAD + length, CW), F32),
            pltpu.VMEM((PAD + length, CW), F32),
            pltpu.VMEM((length + PAD, CW), F32),
            pltpu.VMEM((length + PAD, CW), F32),
            pltpu.VMEM((length, CW), BF16),
            pltpu.VMEM((length, CW), BF16),
            pltpu.VMEM((small_rows, 8, CW), F32),
            pltpu.VMEM((length, width), F32),
            line,
            line,
            line,
            pltpu.VMEM((tp_count, term_rows, width), BF16),
            pltpu.VMEM((tp_count - 1, term_rows, width), BF16),
            pltpu.VMEM((taps, hidden_cols), F32),
            pltpu.VMEM((taps, hidden_cols), F32),
            pltpu.VMEM((hidden_cols,), F32),
            pltpu.VMEM((hidden_cols,), F32),
            small,
            small_line,
            small_line,
            small_line,
            small_line,
            dma((3, SLOTS)),
            dma((8,)),
            dma((WINDOW,)),
            dma((ring,)),
            dma((WINDOW,)),
            dma((ring,)),
            dma((tp_count - 1,)),
            dma((tp_count - 1,)),
            dma((tp_count - 1,)),
            dma((tp_count - 1,)),
            dma((4,)),
        ],
        compiler_params=pltpu.CompilerParams(
            collective_id=0, has_side_effects=True, vmem_limit_bytes=48 * 2**20
        ),
    )(
        tokens,
        gate_pre,
        up_pre,
        hidden_grad,
        gate_weight,
        up_weight,
        gate_taps,
        up_taps,
        gate_bias,
        up_bias,
    )
    held = [pltpu.with_memory_space_constraint(x, pltpu.VMEM) for x in (summed, final, small_sum)]
    return pl.pallas_call(
        spread,
        out_shape=(
            jax.ShapeDtypeStruct((length, width), BF16),
            jax.ShapeDtypeStruct((width, hidden_cols), F32),
            jax.ShapeDtypeStruct((width, hidden_cols), F32),
            jax.ShapeDtypeStruct((taps, hidden_cols), F32),
            jax.ShapeDtypeStruct((taps, hidden_cols), F32),
            jax.ShapeDtypeStruct((hidden_cols,), F32),
            jax.ShapeDtypeStruct((hidden_cols,), F32),
        ),
        in_specs=[vmem] * 3,
        out_specs=[anywhere] * 7,
        scratch_shapes=[
            pltpu.VMEM((NQ, rows_q, hidden_cols), F32),
            pltpu.VMEM((NQ, rows_q, hidden_cols), F32),
            pltpu.VMEM((taps, hidden_cols), F32),
            pltpu.VMEM((taps, hidden_cols), F32),
            pltpu.VMEM((hidden_cols,), F32),
            pltpu.VMEM((hidden_cols,), F32),
            dma((2, NQ)),
            dma((tp_count,)),
            dma((4,)),
        ],
        compiler_params=pltpu.CompilerParams(vmem_limit_bytes=16 * 2**20),
    )(*held)


def solution(mesh):
    return jax.shard_map(
        functools.partial(per_device, mesh.shape["rep"], mesh.shape["tp"]),
        mesh=mesh,
        in_specs=(
            P("rep", "fs"),
            P("rep", "tp"),
            P("rep", "tp"),
            P("rep", "tp"),
            P("fs", "tp"),
            P("fs", "tp"),
            P(None, "tp"),
            P(None, "tp"),
            P("tp"),
            P("tp"),
        ),
        out_specs=(
            P("rep", "fs"),
            P("fs", "tp"),
            P("fs", "tp"),
            P(None, "tp"),
            P(None, "tp"),
            P("tp"),
            P("tp"),
        ),
        check_vma=False,
    )
```
